32 devices in a mesh: sp: 8 (over z, y), tp: 4 (over x, core).
Axes of the slice: x: 2, y: 2, z: 4, core: 2. Of those that a mesh axis runs over, the one named last changes fastest.
Arguments:
- middle_stream: bfloat16 [1536, 2048], P('sp', 'tp'), may hold values from -6 to 6
- output_gradient: bfloat16 [1536, 2048], P('sp', 'tp'), may hold values from -6 to 6
- routes: int32 [1536, 2], P('sp'), may hold values from 0 to 7, all different within a row; in each aligned block of 192 rows (0 to 191, 192 to 383, ...) at most 72 rows name the same one
- chosen_expert_weight: float32 [1536, 2], P('sp'), may hold values from 0.2 to 1
- expert_gate_weight: bfloat16 [8, 2048, 3584], P('sp', None, 'tp'), may hold values from -0.125 to 0.125
- expert_up_weight: bfloat16 [8, 2048, 3584], P('sp', None, 'tp'), may hold values from -0.125 to 0.125
- expert_down_weight: bfloat16 [8, 3584, 2048], P('sp', 'tp'), may hold values from -0.09375 to 0.09375
- recurrent_output_weight: bfloat16 [2048, 1024], P(None, 'tp'), may hold values from -0.1875 to 0.1875
- recurrence_input: bfloat16 [1536, 1024], P('sp', 'tp'), may hold values from -8 to 8
- output_gate_logits: bfloat16 [1536, 1024], P('sp', 'tp'), may hold values from -6 to 6
- recurrence_gate_weight: bfloat16 [8, 128, 128], replicated, may hold values from -0.5 to 0.5
- input_gate_weight: bfloat16 [8, 128, 128], replicated, may hold values from -0.5 to 0.5
- channel_decay_param: float32 [1024], P('tp'), may hold values from 4 to 13
- extra_log_decay: float32 [1536, 1024], P('sp', 'tp'), may hold values from -0.7 to 0
Outputs:
- grad_gate: bfloat16 [8, 2048, 3584], P('sp', None, 'tp')
- grad_up: bfloat16 [8, 2048, 3584], P('sp', None, 'tp')
- grad_down: bfloat16 [8, 3584, 2048], P('sp', 'tp')
- grad_out_proj: float32 [2048, 1024], P('sp', 'tp')
- grad_input: float32 [1536, 1024], P('sp', 'tp')
- grad_gate_pre: float32 [1536, 1024], P('sp', 'tp')
The draws below stay inside these ranges and needn't reach their ends.
Inputs may be any that keep to these rules, and one draw needn't show every extreme that they name: `routes`: in the rows of one index of sp no expert is named more than 72 times, a bound that some block reaches in some of them; the entries of a row differ.
All inputs are finite; a program needn't handle non-finite values.
Results may differ from the reference program's by a relative error of at most 0.017.
Values may be sent and summed in bfloat16 or wider, within the bound.
A program may use at most 128 MiB of HBM per device.

```python
import math
import jax
import jax.numpy as jnp
import numpy as np
from jax import lax

D = 2048
FF = 3584
BLOCKS = 8
BW = 128
TOP = 2
TOK_DEV = 192
CHANNEL_COUNT = 1024
SEQUENCE_TOKENS = 1536
EXPERTS = 8
CAP = 72
N_SP = 8
N_TP = 4


def draw_recurrence_input(key, part):
    initial_key, second_key = jax.random.split(jax.random.fold_in(key, 11))
    base_draw = jnp.clip(jax.random.normal(initial_key, (SEQUENCE_TOKENS, CHANNEL_COUNT), jnp.float32), -4.0, 4.0)
    factor = jnp.exp(jax.random.uniform(second_key, (SEQUENCE_TOKENS // TOK_DEV, 1, 1), jnp.float32, math.log(0.5), math.log(2.0)))
    scaled = (base_draw.reshape(SEQUENCE_TOKENS // TOK_DEV, TOK_DEV, CHANNEL_COUNT) * factor).reshape(SEQUENCE_TOKENS, CHANNEL_COUNT)
    return scaled.astype(jnp.bfloat16)


def draw_channel_decay_param(key, part):
    initial_key, second_key, third_key = jax.random.split(jax.random.fold_in(key, 23), 3)
    fast_share = 0.5
    fast_pick = jax.random.uniform(initial_key, (CHANNEL_COUNT,), jnp.float32) < fast_share
    fast_rate = jnp.exp(jax.random.uniform(second_key, (CHANNEL_COUNT,), jnp.float32, math.log(0.003), math.log(0.01)))
    slow_rate = jnp.exp(jax.random.uniform(third_key, (CHANNEL_COUNT,), jnp.float32, math.log(0.05), math.log(0.3))) / SEQUENCE_TOKENS
    chosen = jnp.where(fast_pick, fast_rate, slow_rate)
    return (-jnp.log(jnp.expm1(chosen))).astype(jnp.float32)


def draw_extra_log_decay(key, part):
    initial_key, second_key = jax.random.split(jax.random.fold_in(key, 37))
    spike_mask = jax.random.uniform(initial_key, (SEQUENCE_TOKENS, CHANNEL_COUNT), jnp.float32) < 4.0 / SEQUENCE_TOKENS
    loss_history = jax.random.uniform(second_key, (SEQUENCE_TOKENS, CHANNEL_COUNT), jnp.float32, math.log(0.5), math.log(0.8))
    return jnp.where(spike_mask, loss_history, 0.0).astype(jnp.float32)


def strengthened(array, key, source, target, shards_of, factor):
    owner, partner = [(jnp.arange(array.shape[axis_at]) // (array.shape[axis_at] // shards_of)).reshape([-1 if axis == axis_at else 1 for axis in range(array.ndim)]) for axis_at in (source, target)]
    chosen = jax.random.permutation(key, shards_of)[partner]
    strong = (owner == chosen) | (owner == (partner + shards_of // 2) % shards_of)
    return jnp.where(strong, factor * array, array)


def steps_of(key, shape, cuts, smallest, top_value):
    loudness = 1.0
    for axis_at, shards_of in cuts:
        draws = jax.random.uniform(jax.random.fold_in(jax.random.fold_in(key, 6), axis_at), (shards_of,), jnp.float32, smallest / len(cuts), top_value / len(cuts))
        loudness = loudness * jnp.repeat(jnp.exp(draws), shape[axis_at] // shards_of).reshape((-1,) + (1,) * (len(shape) - 1 - axis_at))
    return loudness


def shared_out(key, own, number, rows, number_of, top, reach, skew):
    ranking = jax.random.permutation(key, number_of)
    heavy_load, ordinary = portions_of(number_of, rows * top, reach, skew, True), portions_of(number_of, rows * top, reach, skew, False)
    places = jnp.arange(number_of)

    def named(tallies, turn):
        used = int((tallies > 0).sum())
        fixed = max(1, used // 4)
        shifted = fixed + (places - fixed + turn * (used - fixed)) % max(1, number_of - fixed)
        return jnp.zeros((number_of,), jnp.int32).at[ranking[jnp.where(places < fixed, places, shifted)]].set(jnp.asarray(tallies, jnp.int32))

    tallies = jnp.where(number % 4 == 0, named(heavy_load, number // 4), named(ordinary, number - number // 4 - 1))
    mixed = jax.random.permutation(jax.random.fold_in(own, 3), number_of)
    source_of, taker = mixed[0:number_of // 2 * 2:2], mixed[1:number_of // 2 * 2:2]
    slack = jnp.minimum(tallies[source_of] - 1, reach - tallies[taker]) // 2
    slack = jnp.where((source_of == ranking[0]) | (taker == ranking[0]) | (tallies[taker] == 0), 0, jnp.maximum(slack, 0))
    shifted = jax.random.randint(jax.random.fold_in(own, 4), (number_of // 2,), 0, 1 << 20) % (slack + 1)
    tallies = tallies.at[source_of].add(-shifted).at[taker].add(shifted)
    labels = jnp.searchsorted(jnp.cumsum(tallies), jnp.arange(rows * top), side="right").astype(jnp.int32)
    listing = labels.reshape(top, rows).T
    listing = listing[jax.random.permutation(jax.random.fold_in(own, 1), rows)]
    turn = jax.random.randint(jax.random.fold_in(own, 2), (rows, 1), 0, top)
    return jnp.take_along_axis(listing, (jnp.arange(top)[None, :] + turn) % top, axis=1)


def portions_of(amount, total, bound, slope, full):
    portions = [(1 << 20) // math.isqrt(grade ** slope) + 1 for grade in range(1, amount + 1)]
    largest = bound if full else min(bound, max(-(-total // amount), total * portions[0] // sum(portions)))
    least = 1 if total - largest >= amount - 1 else 0
    holding, spare = [largest] + [least] * (amount - 1), total - largest - least * (amount - 1)
    while spare > 0:
        candidates = [i for i in range(1, amount) if holding[i] < largest] or [i for i in range(1, amount) if holding[i] < bound]
        whole, budget = sum([portions[i] for i in candidates]), spare
        for i in candidates:
            more = min(bound - holding[i], max(1, budget * portions[i] // whole), spare)
            holding[i] = holding[i] + more
            spare = spare - more
    return np.array(holding)


def bell_draw(stream_key, dims, width, bound, cuts=(), kind=jnp.bfloat16):
    array = jax.random.normal(stream_key, dims, jnp.float32) * width
    if len(cuts) > 0:
        array = steps_of(stream_key, dims, cuts, -0.22, 0.18) * array
    return jnp.clip(array, min=-bound, max=bound).astype(kind)


def noise_with(rng, dims, width, most, cuts, heavy, kind=jnp.bfloat16):
    array = width * jax.random.normal(rng, dims, jnp.float32)
    if cuts:
        array = array * steps_of(rng, dims, cuts, -0.22, 0.18)
    return jnp.clip(strengthened(array, jax.random.fold_in(rng, 3), *heavy), -most, most).astype(kind)


def setup_inputs(seed: int = 0) -> dict:
    streams_of = jax.random.split(jax.random.key(seed), 15)
    middle_stream = bell_draw(streams_of[0], (SEQUENCE_TOKENS, D), 1.0, 6.0, ((0, 8), (1, 4)))
    output_gradient = noise_with(streams_of[1], (SEQUENCE_TOKENS, D), 1.0, 6.0, ((0, 8), (1, 4)), (0, 1, 8, 2.0))
    routes_keys = jax.random.split(jax.random.fold_in(streams_of[2], 1), SEQUENCE_TOKENS // TOK_DEV)
    routes_turns = jax.random.permutation(jax.random.fold_in(streams_of[2], 3), SEQUENCE_TOKENS // TOK_DEV)
    routes = jax.vmap(lambda own, number: shared_out(jax.random.fold_in(streams_of[2], 2), own, number, TOK_DEV, EXPERTS, TOP, CAP, 1))(routes_keys, routes_turns).reshape((SEQUENCE_TOKENS, TOP))
    chosen_expert_weight = jnp.clip(0.2 + 0.8 * jax.random.uniform(streams_of[3], (SEQUENCE_TOKENS, TOP), jnp.float32) ** steps_of(streams_of[3], (SEQUENCE_TOKENS, TOP), ((0, 8),), -0.2, 0.2), 0.2, 1.0)
    expert_gate_weight = bell_draw(streams_of[4], (EXPERTS, D, FF), D ** -0.5, 0.125, ((0, 8), (2, 4)))
    expert_up_weight = bell_draw(streams_of[5], (EXPERTS, D, FF), D ** -0.5, 0.125, ((0, 8), (2, 4)))
    expert_down_weight = bell_draw(streams_of[6], (EXPERTS, FF, D), FF ** -0.5, 0.09375, ((0, 8), (1, 4)))
    recurrent_output_weight = bell_draw(streams_of[7], (D, CHANNEL_COUNT), CHANNEL_COUNT ** -0.5, 0.1875, ((1, 4),))
    recurrence_input = draw_recurrence_input(jax.random.fold_in(streams_of[14], 71), 0)
    output_gate_logits = bell_draw(streams_of[9], (SEQUENCE_TOKENS, CHANNEL_COUNT), 1.0, 6.0, ((0, 8), (1, 4)))
    recurrence_gate_weight = bell_draw(streams_of[10], (BLOCKS, BW, BW), BW ** -0.5, 0.5)
    input_gate_weight = bell_draw(streams_of[11], (BLOCKS, BW, BW), BW ** -0.5, 0.5)
    channel_decay_param = draw_channel_decay_param(jax.random.fold_in(streams_of[14], 71), 0)
    extra_log_decay = draw_extra_log_decay(jax.random.fold_in(streams_of[14], 71), 0)
    return {"middle_stream": middle_stream, "output_gradient": output_gradient, "routes": routes, "chosen_expert_weight": chosen_expert_weight, "expert_gate_weight": expert_gate_weight, "expert_up_weight": expert_up_weight, "expert_down_weight": expert_down_weight, "recurrent_output_weight": recurrent_output_weight, "recurrence_input": recurrence_input, "output_gate_logits": output_gate_logits, "recurrence_gate_weight": recurrence_gate_weight, "input_gate_weight": input_gate_weight, "channel_decay_param": channel_decay_param, "extra_log_decay": extra_log_decay}


def combine_linear(earlier, latter):
    return (earlier[0] * latter[0], latter[0] * earlier[1] + latter[1])

def linear_scan(factor, driven):
    return lax.associative_scan(combine_linear, (factor, driven), axis=0)

def gelu_parts(output_gate_logits):
    gate_float = output_gate_logits.astype(jnp.float32)
    return jax.jvp(jax.nn.gelu, (gate_float,), (jnp.ones_like(gate_float),))

def expert_backward(inputs, cotangent, gate_weight, up_weight, down_weight):
    gate_act = jnp.dot(inputs, gate_weight, preferred_element_type=jnp.float32)
    up_act = jnp.dot(inputs, up_weight, preferred_element_type=jnp.float32)
    sigmoid_gate = jax.nn.sigmoid(gate_act)
    silu_act = gate_act * sigmoid_gate
    hidden = (silu_act * up_act).astype(jnp.bfloat16)
    d_hidden = lax.dot_general(cotangent, down_weight, (((1,), (1,)), ((), ())), preferred_element_type=jnp.float32)
    grad_down = lax.dot_general(hidden, cotangent, (((0,), (0,)), ((), ())), preferred_element_type=jnp.float32)
    d_gate = (d_hidden * up_act * sigmoid_gate * (1.0 + gate_act * (1.0 - sigmoid_gate))).astype(jnp.bfloat16)
    d_up = (d_hidden * silu_act).astype(jnp.bfloat16)
    grad_gate = lax.dot_general(inputs, d_gate, (((0,), (0,)), ((), ())), preferred_element_type=jnp.float32)
    grad_up = lax.dot_general(inputs, d_up, (((0,), (0,)), ((), ())), preferred_element_type=jnp.float32)
    return (grad_gate.astype(jnp.bfloat16), grad_up.astype(jnp.bfloat16), grad_down.astype(jnp.bfloat16), d_gate, d_up)

def reference(middle_stream, output_gradient, routes, chosen_expert_weight, expert_gate_weight, expert_up_weight, expert_down_weight, recurrent_output_weight, recurrence_input, output_gate_logits, recurrence_gate_weight, input_gate_weight, channel_decay_param, extra_log_decay):
    tokens, model_width = middle_stream.shape
    top_count = routes.shape[1]
    routed = routes.reshape(-1)
    onehot = (routed[:, None] == jnp.arange(EXPERTS, dtype=jnp.int32)[None, :]).astype(jnp.int32)
    onehot = onehot.reshape(N_SP, TOK_DEV * top_count, EXPERTS)
    slot_rank = (lax.optimization_barrier(jnp.sum(jnp.cumsum(onehot, axis=1) * onehot, axis=2)) - 1).reshape(-1)
    source = jnp.arange(tokens * top_count, dtype=jnp.int32) // (TOK_DEV * top_count)
    buffer_place = (source * CAP + slot_rank).astype(jnp.int32)
    slot_table = jnp.full((EXPERTS, N_SP * CAP), tokens * top_count, jnp.int32)
    slot_table = slot_table.at[routed, buffer_place].set(jnp.arange(tokens * top_count, dtype=jnp.int32))
    zero_row = jnp.zeros((1, model_width), jnp.bfloat16)
    pair_rows = jnp.broadcast_to(middle_stream[:, None, :], (tokens, top_count, model_width)).reshape(-1, model_width)
    pair_rows = jnp.concatenate([pair_rows, zero_row], axis=0)
    pair_cot = (chosen_expert_weight[:, :, None] * output_gradient.astype(jnp.float32)[:, None, :]).astype(jnp.bfloat16)
    pair_cot = jnp.concatenate([pair_cot.reshape(-1, model_width), zero_row], axis=0)

    def one_expert(packed):
        table_row, gate_weight, up_weight, down_weight = packed
        inputs = pair_rows[table_row]
        cotangent = pair_cot[table_row]
        grad_gate, grad_up, grad_down, d_gate, d_up = expert_backward(inputs, cotangent, gate_weight, up_weight, down_weight)
        slot_rows = inputs.shape[0]
        quarter = gate_weight.shape[1] // N_TP
        gate_q = d_gate.astype(jnp.float32).reshape(slot_rows, N_TP, quarter)
        up_q = d_up.astype(jnp.float32).reshape(slot_rows, N_TP, quarter)
        gate_wq = gate_weight.astype(jnp.float32).reshape(model_width, N_TP, quarter)
        up_wq = up_weight.astype(jnp.float32).reshape(model_width, N_TP, quarter)
        partial_value = jnp.einsum('rqf,dqf->qrd', gate_q, gate_wq) + jnp.einsum('rqf,dqf->qrd', up_q, up_wq)
        rounded = lax.optimization_barrier(partial_value.astype(jnp.bfloat16)).astype(jnp.float32)
        slot_grad = lax.optimization_barrier(jnp.sum(rounded, axis=0)).astype(jnp.bfloat16)
        return (grad_gate, grad_up, grad_down, slot_grad)
    grad_gate, grad_up, grad_down, slot_grad = lax.map(one_expert, (slot_table, expert_gate_weight, expert_up_weight, expert_down_weight))
    slot_back = jnp.zeros((tokens * top_count + 1, model_width), jnp.bfloat16)
    slot_back = slot_back.at[slot_table.reshape(-1)].set(slot_grad.reshape(-1, model_width))
    arrived = slot_back[:-1].astype(jnp.float32).reshape(tokens, top_count, model_width)
    residual_grad = (output_gradient.astype(jnp.float32) + lax.optimization_barrier(jnp.sum(arrived, axis=1))).astype(jnp.bfloat16)
    mixer_grad = jnp.dot(residual_grad, recurrent_output_weight, preferred_element_type=jnp.float32)
    channels = recurrence_input.shape[1]
    blocks, block_width = (recurrence_gate_weight.shape[0], recurrence_gate_weight.shape[1])
    u_float = recurrence_input.astype(jnp.float32)
    u_blocks = u_float.reshape(tokens, blocks, block_width)
    forget_gate = jax.nn.sigmoid(jnp.einsum('tnb,nbc->tnc', u_blocks, recurrence_gate_weight.astype(jnp.float32)).reshape(tokens, channels))
    admit_gate = jax.nn.sigmoid(jnp.einsum('tnb,nbc->tnc', u_blocks, input_gate_weight.astype(jnp.float32)).reshape(tokens, channels))
    baseline_rate = jax.nn.softplus(-channel_decay_param)
    decay_logarithm = -8.0 * forget_gate * baseline_rate[None, :] + extra_log_decay
    decay_step = jnp.exp(decay_logarithm)
    input_scale = jnp.sqrt(-jnp.expm1(2.0 * decay_logarithm))
    driven = u_float * admit_gate * input_scale
    _, states = linear_scan(decay_step, driven)
    prev_states = jnp.concatenate([jnp.zeros((1, channels), jnp.float32), states[:-1]], axis=0)
    gelu_val, gelu_der = gelu_parts(output_gate_logits)
    lru_out = (states * gelu_val).astype(jnp.bfloat16)
    grad_out_proj = lax.dot_general(residual_grad, lru_out, (((0,), (0,)), ((), ())), preferred_element_type=jnp.float32)
    grad_gate_pre = mixer_grad * states * gelu_der
    state_in = mixer_grad * gelu_val
    next_decay = jnp.concatenate([decay_step[1:], jnp.zeros((1, channels), jnp.float32)], axis=0)
    _, flipped = linear_scan(next_decay[::-1], state_in[::-1])
    state_grad = flipped[::-1]
    d_log = state_grad * (prev_states * decay_step - u_float * admit_gate * decay_step * decay_step / input_scale)
    d_recall = (d_log * (-8.0 * baseline_rate[None, :]) * forget_gate * (1.0 - forget_gate)).astype(jnp.bfloat16)
    d_admit = (state_grad * u_float * input_scale * admit_gate * (1.0 - admit_gate)).astype(jnp.bfloat16)
    back_recall = jnp.einsum('tnc,nbc->tnb', d_recall.astype(jnp.float32).reshape(tokens, blocks, block_width), recurrence_gate_weight.astype(jnp.float32))
    back_admit = jnp.einsum('tnc,nbc->tnb', d_admit.astype(jnp.float32).reshape(tokens, blocks, block_width), input_gate_weight.astype(jnp.float32))
    grad_input = state_grad * admit_gate * input_scale + (back_recall + back_admit).reshape(tokens, channels)
    return (grad_gate, grad_up, grad_down, grad_out_proj, grad_input, grad_gate_pre)
```

```python
import functools

import jax
import jax.numpy as jnp
from jax import lax
from jax.experimental import pallas as pl
from jax.experimental.pallas import tpu as pltpu
from jax.sharding import PartitionSpec as P

MESH = pl.DeviceIdType.MESH


def partner(t, stage, m):
    d = m >> (stage + 1)
    return t + d * (1 - 2 * ((t // d) % 2))


def flipped(s, j, n):
    out = 0
    for b in range(n.bit_length() - 1):
        bit = (s // 2**b) % 2
        out = out + (1 - bit if (j >> b) % 2 else bit) * 2**b
    return out


def far_near(n):
    near, far = list(range(n // 2)), list(range(n // 2, n))
    arrive = near[:1]
    for i in range(1, n // 2):
        arrive += [near[i], far[i - 1]]
    leave = []
    for i in range(1, n // 2):
        leave += [far[i - 1], near[i]]
    return arrive + far[-1:], leave + far[-1:], far + near[1:] + near[:1]


def held_columns(t, stage, m):
    if stage == 0:
        return [t]
    return held_columns(t, stage - 1, m) + held_columns(partner(t, stage - 1, m), stage - 1, m)


def greet(peers):
    barrier = pltpu.get_barrier_semaphore()
    for peer in peers:
        pl.semaphore_signal(barrier, inc=1, device_id=peer, device_id_type=MESH)
    pl.semaphore_wait(barrier, len(peers))


def remote(src, dst, send_sem, recv_sem, peer):
    return pltpu.make_async_remote_copy(
        src_ref=src,
        dst_ref=dst,
        send_sem=send_sem,
        recv_sem=recv_sem,
        device_id=peer,
        device_id_type=MESH,
    )


def shifted(value, k, fill, reverse):
    pad = jnp.full((k, value.shape[1]), fill, value.dtype)
    if reverse:
        return jnp.concatenate([value[k:], pad], axis=0)
    return jnp.concatenate([pad, value[:-k]], axis=0)


def local_scan(gain, term, reverse):
    k = 1
    while k < gain.shape[0]:
        term = term + gain * shifted(term, k, 0.0, reverse)
        gain = gain * shifted(gain, k, 1.0, reverse)
        k *= 2
    return gain, term


def dispatch_kernel(
    n,
    m,
    rows_ref,
    cot_ref,
    decay_ref,
    driven_ref,
    rows_out,
    cot_out,
    states_ref,
    prev_ref,
    gain_buf,
    car_send,
    car_buf,
    a2a_send,
    a2a_recv,
    tp_send,
    tp_recv,
    car_ssem,
    car_rsem,
    self_sem,
):
    sources, targets = (rows_ref, cot_ref), (rows_out, cot_out)
    s, t = lax.axis_index("sp"), lax.axis_index("tp")
    feat = rows_ref.shape[2]
    stages = m.bit_length() - 1
    greet(
        [{"sp": lax.rem(s + k, n)} for k in range(1, n)]
        + [{"tp": partner(t, j, m)} for j in range(stages)]
    )

    def block(a, src, col):
        return targets[a].at[src, :, pl.ds(pl.multiple_of(col * feat, feat), feat)]

    first = {}
    arrive, leave, _ = far_near(n)
    for k in [0] + leave:
        dst = flipped(s, k, n)
        for a in range(2):
            if k == 0:
                copy = pltpu.make_async_copy(sources[a].at[s], block(a, s, t), self_sem.at[a])
            else:
                copy = remote(
                    sources[a].at[dst],
                    block(a, s, t),
                    a2a_send.at[a, k],
                    a2a_recv.at[a, k],
                    {"sp": dst},
                )
            copy.start()
            first[k, a] = copy

    pushed = []

    def push(a, k, stage, i, col):
        src = flipped(s, k, n)
        at = 2**stage - 1 + i
        copy = remote(
            block(a, src, col),
            block(a, src, col),
            tp_send.at[a, at, k],
            tp_recv.at[a, at, k],
            {"tp": partner(t, stage, m)},
        )
        copy.start()
        pushed.append(copy)

    def arrived(k, stage):
        src = flipped(s, k, n)
        cols = held_columns(partner(t, stage, m), stage, m)
        for i, col in enumerate(cols):
            at = 2**stage - 1 + i
            for a in range(2):
                remote(
                    block(a, src, col),
                    block(a, src, col),
                    tp_send.at[a, at, k],
                    tp_recv.at[a, at, k],
                    {"tp": partner(t, stage, m)},
                ).wait_recv()
                for later in range(stage + 1, stages):
                    push(a, k, later, 2**stage + i, col)

    def forward(k):
        for a in range(2):
            if k == 0:
                first[k, a].wait()
            else:
                first[k, a].wait_recv()
            for stage in range(stages):
                push(a, k, stage, 0, t)

    forward(arrive[0])
    gain, term = local_scan(decay_ref[...], driven_ref[...], False)
    gain_buf[...] = gain
    states_ref[...] = term
    rows = gain.shape[0]
    car_send[0:1] = gain[rows - 1 : rows]
    car_send[1:2] = term[rows - 1 : rows]
    forward(arrive[1])
    carries = []
    for k in range(1, n):
        copy = remote(
            car_send, car_buf.at[k], car_ssem.at[k], car_rsem.at[k], {"sp": lax.rem(s + k, n)}
        )
        copy.start()
        carries.append(copy)
    for at in range(2, n):
        forward(arrive[at])
        for stage in range(stages - 1):
            arrived(arrive[at - 2], stage)
    for copy in carries:
        copy.wait()
    carry = jnp.zeros((1, gain_buf.shape[1]), jnp.float32)
    for k in range(n - 1, 0, -1):
        carry = jnp.where(k <= s, car_buf[k, 0:1] * carry + car_buf[k, 1:2], carry)
    states = states_ref[...] + gain_buf[...] * carry
    states_ref[...] = states
    prev_ref[...] = jnp.concatenate([carry, states[:-1]], axis=0)
    for k in arrive[n - 2 :]:
        for stage in range(stages - 1):
            arrived(k, stage)
    for k in range(n):
        arrived(k, stages - 1)
    for k in leave:
        for a in range(2):
            first[k, a].wait_send()
    for copy in pushed:
        copy.wait_send()


def dispatch(send_rows, send_cot, decay, driven):
    n, m = lax.axis_size("sp"), lax.axis_size("tp")
    _, cap, feat = send_rows.shape
    whole = jax.ShapeDtypeStruct((n, cap, m * feat), send_rows.dtype)
    rows, channels = decay.shape
    vmem = pl.BlockSpec(memory_space=pltpu.VMEM)
    state = jax.ShapeDtypeStruct((rows, channels), jnp.float32)
    return pl.pallas_call(
        functools.partial(dispatch_kernel, n, m),
        out_shape=(whole, whole, state, state),
        in_specs=[vmem] * 4,
        out_specs=(vmem,) * 4,
        scratch_shapes=[
            pltpu.VMEM((rows, channels), jnp.float32),
            pltpu.VMEM((2, channels), jnp.float32),
            pltpu.VMEM((n, 2, channels), jnp.float32),
            pltpu.SemaphoreType.DMA((2, n)),
            pltpu.SemaphoreType.DMA((2, n)),
            pltpu.SemaphoreType.DMA((2, m - 1, n)),
            pltpu.SemaphoreType.DMA((2, m - 1, n)),
            pltpu.SemaphoreType.DMA((n,)),
            pltpu.SemaphoreType.DMA((n,)),
            pltpu.SemaphoreType.DMA((2,)),
        ],
        compiler_params=pltpu.CompilerParams(collective_id=0, has_side_effects=True),
        name="dispatch",
    )(send_rows, send_cot, decay, driven)


def gelu_parts(logits):
    x = logits.astype(jnp.float32)
    square = x * x
    slope = 0.7978845608028654
    th = jnp.tanh(slope * (x + 0.044715 * (x * square)))
    value = 0.5 * x * (1.0 + th)
    inner = slope * (1.0 + 3.0 * 0.044715 * square)
    return value, 0.5 * (1.0 + th) + 0.5 * x * (1.0 - th * th) * inner


def dot_f32(a, b):
    return jnp.dot(a, b, preferred_element_type=jnp.float32)


def dot_rows(a, b):
    return lax.dot_general(
        a, b, (((0,), (0,)), ((), ())), preferred_element_type=jnp.float32
    )


def dot_cols(a, b):
    return lax.dot_general(
        a, b, (((1,), (1,)), ((), ())), preferred_element_type=jnp.float32
    )


def expert_kernel(
    n,
    m,
    x_hbm,
    c_hbm,
    wg_hbm,
    wu_hbm,
    wd_hbm,
    wo_hbm,
    pick_ref,
    cot_ref,
    states_ref,
    prev_ref,
    decay_ref,
    forget_ref,
    admit_ref,
    scale_ref,
    u_ref,
    logits_ref,
    base_ref,
    rw_ref,
    aw_ref,
    gg_ref,
    gu_ref,
    gd_ref,
    gop_ref,
    gin_ref,
    ggp_ref,
    x_ref,
    c_ref,
    wg_ref,
    wu_ref,
    wd_ref,
    wo_ref,
    hid_ref,
    dg_ref,
    du_ref,
    part_ref,
    acc_ref,
    in_buf,
    home_buf,
    back_buf,
    resid_ref,
    lru_ref,
    blk_ref,
    gop_buf,
    val_ref,
    gains_ref,
    full_gain,
    term_ref,
    co_state,
    co_in,
    co_recall,
    co_admit,
    co_direct,
    car_send,
    car_buf,
    ld_sem,
    rs_send,
    rs_recv,
    a2a_send,
    a2a_recv,
    ag_send,
    ag_recv,
    up_send,
    up_recv,
    dn_send,
    dn_recv,
    lo_send,
    lo_recv,
    blk_send,
    blk_recv,
    bt_send,
    bt_recv,
    car_ssem,
    car_rsem,
):
    s, t = lax.axis_index("sp"), lax.axis_index("tp")
    stages = m.bit_length() - 1
    groups = n // 2
    hi, lo = s // 2, s % 2
    other = 1 - lo
    group_rows = x_ref.shape[0] // groups
    cap = group_rows // 2
    width = x_ref.shape[1]
    hidden = hid_ref.shape[1]
    rows, feat = cot_ref.shape
    channels = states_ref.shape[1]
    quarter = rows // m

    def across(stage):
        d = 2**stage
        return t + d * (1 - 2 * ((t // d) % 2))

    def cols(col):
        return pl.ds(pl.multiple_of(col * feat, feat), feat)

    def at_group(q):
        return pl.ds(pl.multiple_of(q * group_rows, 16), group_rows)

    def at_rows(src):
        return pl.ds(pl.multiple_of(src * rows, 16), rows)

    order = [groups - 1 - j for j in range(groups)]
    place = [flipped(hi, f, groups) for f in order]

    loads = {}

    def load(name, src, dst, at):
        copy = pltpu.make_async_copy(src, dst, ld_sem.at[at])
        copy.start()
        loads[name] = copy

    for j in range(groups):
        load(("x", j), x_hbm.at[at_group(place[j])], x_ref.at[at_group(place[j])], j)
        if j == 0:
            load("g", wg_hbm, wg_ref, 2 * groups)
            load("u", wu_hbm, wu_ref, 2 * groups + 1)
            load(("c", 0), c_hbm.at[at_group(place[0])], c_ref.at[at_group(place[0])], groups)
            load("d", wd_hbm, wd_ref, 2 * groups + 2)
        else:
            load(("c", j), c_hbm.at[at_group(place[j])], c_ref.at[at_group(place[j])], groups + j)
    load("o", wo_hbm, wo_ref, 2 * groups + 3)

    greet(
        [{"sp": lax.rem(s + k, n)} for k in range(1, n)] + [{"tp": across(j)} for j in range(stages)]
    )

    gelu_val, gelu_der = gelu_parts(logits_ref[...])
    states = states_ref[...]
    lru_ref[at_rows(s), :] = (states * gelu_val).astype(jnp.bfloat16)
    co_in[...] = gelu_val
    co_state[...] = states * gelu_der

    def line(step, up):
        src = hi - step if up else hi + step
        block = at_rows(src * 2 + lo)
        peer = hi + 1 if up else hi - 1
        return remote(
            lru_ref.at[block],
            lru_ref.at[block],
            (up_send if up else dn_send).at[step],
            (up_recv if up else dn_recv).at[step],
            {"sp": peer * 2 + lo},
        )

    def beside(src_hi):
        block = at_rows(src_hi * 2 + lo)
        return remote(
            lru_ref.at[block],
            lru_ref.at[block],
            lo_send.at[src_hi],
            lo_recv.at[src_hi],
            {"sp": hi * 2 + other},
        )

    def line_send(step):
        @pl.when((hi >= step) & (hi < groups - 1))
        def _():
            line(step, True).start()

        @pl.when((hi + step < groups) & (hi > 0))
        def _():
            line(step, False).start()

    def line_step(step):
        @pl.when(hi > step)
        def _():
            line(step, True).wait_recv()
            beside(hi - 1 - step).start()

        @pl.when(hi + step < groups - 1)
        def _():
            line(step, False).wait_recv()
            beside(hi + 1 + step).start()

        if step + 1 < groups - 1:
            line_send(step + 1)

    def line_end():
        for step in range(groups - 1):
            @pl.when((hi >= step) & (hi < groups - 1))
            def _():
                line(step, True).wait_send()

            @pl.when((hi + step < groups) & (hi > 0))
            def _():
                line(step, False).wait_send()

        for src_hi in range(groups):
            beside(src_hi).wait()

    line_send(0)
    beside(hi).start()

    base = []
    total = 0
    for stage in range(stages):
        base.append(total)
        total += m >> (stage + 1)
    waits = []

    def send_stage(q, stage):
        source = part_ref if stage == 0 else acc_ref
        step = 2 ** (stage + 1)
        for i in range(m // step):
            col = lax.rem(across(stage) + i * step, m)
            copy = stage_copy(q, stage, i, col, source)
            copy.start()
            waits.append(copy)

    def stage_copy(q, stage, i, col, source):
        at = base[stage] + i
        return remote(
            source.at[at_group(q), cols(col)],
            in_buf.at[at, q],
            rs_send.at[at, q],
            rs_recv.at[at, q],
            {"tp": across(stage)},
        )

    def sum_stage(q, stage):
        source = part_ref if stage == 0 else acc_ref
        step = 2 ** (stage + 1)
        value = None
        for i in range(m // step):
            col = lax.rem(t + i * step, m)
            stage_copy(q, stage, i, col, source).wait_recv()
            value = source[at_group(q), cols(col)].astype(jnp.float32)
            value = value + in_buf[base[stage] + i, q].astype(jnp.float32)
            if stage + 1 < stages:
                acc_ref[at_group(q), cols(col)] = value.astype(jnp.bfloat16)
        return value

    def home_copy(k):
        dst = flipped(s, k, n)
        return remote(
            home_buf.at[dst], back_buf.at[s], a2a_send.at[k], a2a_recv.at[k], {"sp": dst}
        )

    def middle(j):
        for stage in range(stages - 1):
            sum_stage(place[j], stage)
            send_stage(place[j], stage + 1)

    def finish(j):
        value = sum_stage(place[j], stages - 1)
        q = place[j]
        for half in range(2):
            home_buf[2 * q + half] = value[half * cap : (half + 1) * cap].astype(jnp.bfloat16)
        for k in (2 * order[j], 2 * order[j] + 1):
            if k > 0:
                copy = home_copy(k)
                copy.start()
                waits.append(copy)

    tile = 256
    cuts = [(f, min(tile, hidden - f)) for f in range(0, hidden, tile)]

    def forward(j):
        block = at_group(place[j])
        for f0, size in cuts:
            f = pl.ds(f0, size)
            if j == 0 and f0 == 0:
                loads["x", 0].wait()
                loads["g"].wait()
            gate_act = dot_f32(x_ref[block, :], wg_ref[:, f])
            if j == 0 and f0 == 0:
                loads["u"].wait()
            up_act = dot_f32(x_ref[block, :], wu_ref[:, f])
            if j == 0 and f0 == 0:
                loads["c", 0].wait()
                loads["d"].wait()
            d_hidden = dot_cols(c_ref[block, :], wd_ref[f, :])
            sig = jax.nn.sigmoid(gate_act)
            silu = gate_act * sig
            hid_ref[block, f] = (silu * up_act).astype(jnp.bfloat16)
            du_ref[block, f] = (d_hidden * silu).astype(jnp.bfloat16)
            dg_ref[block, f] = (
                d_hidden * up_act * sig * (1.0 + gate_act * (1.0 - sig))
            ).astype(jnp.bfloat16)

    def partial(j, first, last):
        block = at_group(place[j])

        def body(i, carry):
            step = i // (m // 2)
            col = lax.rem(across(0) + step * (t - across(0)) + 2 * lax.rem(i, m // 2) + m, m)
            value = dot_cols(dg_ref[block, :], wg_ref[cols(col), :])
            value = value + dot_cols(du_ref[block, :], wu_ref[cols(col), :])
            part_ref[block, cols(col)] = value.astype(jnp.bfloat16)
            return carry

        lax.fori_loop(first, last, body, 0)

    for j in range(groups):
        if j > 0:
            loads["x", j].wait()
            loads["c", j].wait()
        forward(j)
        if j < groups - 1:
            line_step(j)
        if j > 0:
            middle(j - 1)
        if j > 1:
            finish(j - 2)
        partial(j, 0, m // 2)
        send_stage(place[j], 0)
        partial(j, m // 2, m)

    x_tiles = width // tile
    h_tiles = hidden // 128
    work = [("x", i) for i in range(x_tiles)] + [("h", i) for i in range(h_tiles)]
    done = [0]

    def x_body(i, carry):
        c = pl.ds(pl.multiple_of(i * tile, tile), tile)
        left = x_ref[:, c]
        gg_ref[c, :] = dot_rows(left, dg_ref[...]).astype(jnp.bfloat16)
        gu_ref[c, :] = dot_rows(left, du_ref[...]).astype(jnp.bfloat16)
        return carry

    def h_body(i, carry):
        c = pl.ds(pl.multiple_of(i * 128, 128), 128)
        gd_ref[c, :] = dot_rows(hid_ref[:, c], c_ref[...]).astype(jnp.bfloat16)
        return carry

    def weight_tiles(count):
        stop = min(done[0] + count, x_tiles + h_tiles)
        x_stop = min(stop, x_tiles)
        if done[0] < x_stop:
            lax.fori_loop(done[0], x_stop, x_body, 0)
            done[0] = x_stop
        if done[0] < stop:
            lax.fori_loop(done[0] - x_tiles, stop - x_tiles, h_body, 0)
            done[0] = stop

    last = groups - 1
    weight_tiles(1)
    middle(last)
    if last > 0:
        finish(last - 1)
    decay = decay_ref[...]
    gain = shifted(decay, 1, 1.0, True)
    k = 1
    step = 0
    while k < rows:
        gains_ref[step] = gain
        gain = gain * shifted(gain, k, 1.0, True)
        k *= 2
        step += 1
    full_gain[...] = gain
    forget = forget_ref[...]
    admit = admit_ref[...]
    scale = scale_ref[...]
    u = u_ref[...].astype(jnp.float32)
    co_direct[...] = admit * scale
    co_admit[...] = u * scale * admit * (1.0 - admit)
    d_log = prev_ref[...] * decay - u * admit * decay * decay / scale
    co_recall[...] = d_log * (-8.0 * base_ref[...]) * forget * (1.0 - forget)
    weight_tiles(2)
    finish(last)
    val_ref[...] = cot_ref[...].astype(jnp.float32)

    def collect(k):
        src = flipped(s, k, n)
        if k > 0:
            home_copy(k).wait_recv()
            part = back_buf[src]
        else:
            part = home_buf[s]
        val_ref[...] += dot_f32(pick_ref[src], part)

    for k in range(n - 1, 3, -1):
        collect(k)
    weight_tiles(1)
    for k in range(min(3, n - 1), -1, -1):
        collect(k)
    resid_ref[:, cols(t)] = val_ref[...].astype(jnp.bfloat16)

    def share(stage, i, col):
        at = 2**stage - 1 + i
        return remote(
            resid_ref.at[:, cols(col)],
            resid_ref.at[:, cols(col)],
            ag_send.at[at],
            ag_recv.at[at],
            {"tp": partner(t, stage, m)},
        )

    def push(stage, i, col):
        copy = share(stage, i, col)
        copy.start()
        waits.append(copy)

    for stage in range(stages):
        push(stage, 0, t)
    weight_tiles(5)
    for stage in range(stages):
        for i, col in enumerate(held_columns(partner(t, stage, m), stage, m)):
            share(stage, i, col).wait_recv()
            for later in range(stage + 1, stages):
                push(later, 2**stage + i, col)

    bw = blk_ref.shape[1]
    own = width // n

    def block_cols(index):
        return pl.ds(pl.multiple_of(index * own // bw * bw, bw), bw)

    def piece(src, at):
        start = src * rows + at * quarter
        return pl.ds(pl.multiple_of(start, 16), quarter)

    def block_copy(k):
        dst = flipped(s, k, n)
        return remote(
            resid_ref.at[pl.ds(pl.multiple_of(t * quarter, 16), quarter), block_cols(dst)],
            blk_ref.at[piece(s, t)],
            blk_send.at[k],
            blk_recv.at[k],
            {"sp": dst},
        )

    def pass_copy(k, stage, i, at):
        src = flipped(s, k, n)
        spot = 2**stage - 1 + i
        return remote(
            blk_ref.at[piece(src, at)],
            blk_ref.at[piece(src, at)],
            bt_send.at[spot, k],
            bt_recv.at[spot, k],
            {"tp": partner(t, stage, m)},
        )

    def pass_on(k, stage, i, at):
        copy = pass_copy(k, stage, i, at)
        copy.start()
        waits.append(copy)

    def pass_arrived(k, stage):
        for i, at in enumerate(held_columns(partner(t, stage, m), stage, m)):
            pass_copy(k, stage, i, at).wait_recv()
            for later in range(stage + 1, stages):
                pass_on(k, later, 2**stage + i, at)

    arrive, leave, _ = far_near(n)
    for k in leave:
        copy = block_copy(k)
        copy.start()
        waits.append(copy)
    blk_ref[at_rows(s), :] = resid_ref[:, block_cols(s)]
    loads["o"].wait()
    mixer = dot_f32(resid_ref[...], wo_ref[...])
    ggp_ref[...] = mixer * co_state[...]
    term = mixer * co_in[...]
    k = 1
    step = 0
    while k < rows:
        term = term + gains_ref[step] * shifted(term, k, 0.0, True)
        k *= 2
        step += 1
    term_ref[...] = term
    first_decay = decay_ref[0:1]
    car_send[0:1] = first_decay * full_gain[0:1]
    car_send[1:2] = first_decay * term[0:1]
    carries = []
    for k in range(1, n):
        copy = remote(
            car_send, car_buf.at[k], car_ssem.at[k], car_rsem.at[k], {"sp": lax.rem(s + k, n)}
        )
        copy.start()
        carries.append(copy)
    inbound = arrive[1:]
    for at in range(len(inbound)):
        block_copy(inbound[at]).wait_recv()
        for stage in range(stages):
            pass_on(inbound[at], stage, 0, t)
        if at == len(inbound) // 2:
            weight_tiles(x_tiles + h_tiles)
    line_end()
    for copy in carries:
        copy.wait()
    carry = jnp.zeros((1, channels), jnp.float32)
    for k in range(1, n):
        carry = jnp.where(k > s, car_buf[k, 0:1] * carry + car_buf[k, 1:2], carry)
    for k in inbound:
        for stage in range(stages - 1):
            pass_arrived(k, stage)
    state_grad = term_ref[...] + full_gain[...] * carry
    d_recall = (state_grad * co_recall[...]).astype(jnp.bfloat16)
    d_admit = (state_grad * co_admit[...]).astype(jnp.bfloat16)
    direct = state_grad * co_direct[...]
    lane = rw_ref.shape[1]
    local = channels // lane
    for b in range(local):
        c = slice(b * lane, (b + 1) * lane)
        gin_ref[:, c] = (
            direct[:, c]
            + dot_cols(d_recall[:, c], rw_ref[t * local + b])
            + dot_cols(d_admit[:, c], aw_ref[t * local + b])
        )
    for k in inbound:
        pass_arrived(k, stages - 1)
    gop_buf[...] = dot_rows(blk_ref[...], lru_ref[...])
    start = lax.rem(s * own, bw)
    gop_ref[...] = gop_buf[pl.ds(pl.multiple_of(start, 8), own), :]
    for copy in waits:
        copy.wait_send()


def expert_step(rows_in, cot_in, weights, pick, cot, recurrent):
    n, m = lax.axis_size("sp"), lax.axis_size("tp")
    total, width = rows_in.shape
    hidden = weights[2].shape[0]
    rows, feat = cot.shape
    channels = recurrent[0].shape[1]
    cap = total // n
    groups = n // 2
    own = width // n
    bw = max(128, own)
    levels = (rows - 1).bit_length()
    bf16, f32 = jnp.bfloat16, jnp.float32
    vmem = pl.BlockSpec(memory_space=pltpu.VMEM)
    hbm = pl.BlockSpec(memory_space=pl.ANY)
    dma = pltpu.SemaphoreType.DMA
    state = pltpu.VMEM((rows, channels), f32)
    return pl.pallas_call(
        functools.partial(expert_kernel, n, m),
        out_shape=(
            pltpu.VMEM((width, hidden), bf16),
            pltpu.VMEM((width, hidden), bf16),
            pltpu.VMEM((hidden, width), bf16),
            pltpu.VMEM((own, channels), f32),
            pltpu.VMEM((rows, channels), f32),
            pltpu.VMEM((rows, channels), f32),
        ),
        in_specs=[hbm] * 6 + [vmem] * (2 + len(recurrent)),
        out_specs=(vmem,) * 6,
        scratch_shapes=[
            pltpu.VMEM((total, width), bf16),
            pltpu.VMEM((total, width), bf16),
            pltpu.VMEM((width, hidden), bf16),
            pltpu.VMEM((width, hidden), bf16),
            pltpu.VMEM((hidden, width), bf16),
            pltpu.VMEM((width, channels), bf16),
            pltpu.VMEM((total, hidden), bf16),
            pltpu.VMEM((total, hidden), bf16),
            pltpu.VMEM((total, hidden), bf16),
            pltpu.VMEM((total, width), bf16),
            pltpu.VMEM((total, width), bf16),
            pltpu.VMEM((m - 1, groups, 2 * cap, feat), bf16),
            pltpu.VMEM((n, cap, feat), bf16),
            pltpu.VMEM((n, cap, feat), bf16),
            pltpu.VMEM((rows, width), bf16),
            pltpu.VMEM((n * rows, channels), bf16),
            pltpu.VMEM((n * rows, bw), bf16),
            pltpu.VMEM((bw, channels), f32),
            pltpu.VMEM((rows, feat), f32),
            pltpu.VMEM((levels, rows, channels), f32),
            state,
            state,
            state,
            state,
            state,
            state,
            state,
            pltpu.VMEM((2, channels), f32),
            pltpu.VMEM((n, 2, channels), f32),
            dma((2 * groups + 4,)),
            dma((m - 1, groups)),
            dma((m - 1, groups)),
            dma((n,)),
            dma((n,)),
            dma((m - 1,)),
            dma((m - 1,)),
            dma((groups,)),
            dma((groups,)),
            dma((groups,)),
            dma((groups,)),
            dma((groups,)),
            dma((groups,)),
            dma((n,)),
            dma((n,)),
            dma((m - 1, n)),
            dma((m - 1, n)),
            dma((n,)),
            dma((n,)),
        ],
        compiler_params=pltpu.CompilerParams(
            collective_id=1, has_side_effects=True, vmem_limit_bytes=44 * 2**20
        ),
        name="expert_step",
    )(rows_in, cot_in, *weights, pick, cot, *recurrent)


def per_device(
    middle_stream,
    output_gradient,
    routes,
    chosen_expert_weight,
    expert_gate_weight,
    expert_up_weight,
    expert_down_weight,
    recurrent_output_weight,
    recurrence_input,
    output_gate_logits,
    recurrence_gate_weight,
    input_gate_weight,
    channel_decay_param,
    extra_log_decay,
):
    rows_dev = middle_stream.shape[0]
    top_count = routes.shape[1]
    experts = lax.axis_size("sp")
    capacity = -(-3 * top_count * rows_dev // (2 * experts))
    capacity = -(-capacity // 8) * 8
    feat_width = middle_stream.shape[1]
    choice = routes.T
    expert_ids = jnp.arange(experts, dtype=jnp.int32)
    named = [(choice[k][None, :] == expert_ids[:, None]) for k in range(top_count)]
    named_any = sum(part.astype(jnp.bfloat16) for part in named)
    position = jnp.arange(rows_dev, dtype=jnp.int32)
    earlier = (position[:, None] < position[None, :]).astype(jnp.bfloat16)
    rank = jnp.dot(named_any, earlier, preferred_element_type=jnp.float32).astype(jnp.int32)
    slot_ids = jnp.arange(experts * capacity, dtype=jnp.int32)
    picks = []
    for k in range(top_count):
        slot = jnp.sum(
            jnp.where(named[k], rank + expert_ids[:, None] * capacity, 0), axis=0, keepdims=True
        )
        picks.append((slot_ids[:, None] == slot).astype(jnp.bfloat16))
    pick_any = sum(picks)
    pick_both = jnp.concatenate(picks, axis=1)
    pair_cot = (
        chosen_expert_weight.T[:, :, None] * output_gradient.astype(jnp.float32)[None]
    ).astype(jnp.bfloat16)
    pair_cot = pair_cot.reshape(-1, feat_width)
    send_rows = jnp.dot(pick_any, middle_stream, preferred_element_type=jnp.bfloat16)
    send_cot = jnp.dot(pick_both, pair_cot, preferred_element_type=jnp.bfloat16)
    channels = recurrence_input.shape[1]
    block_width = recurrence_gate_weight.shape[1]
    local_blocks = channels // block_width
    first_block = lax.axis_index("tp") * local_blocks
    recall_weight = lax.dynamic_slice_in_dim(recurrence_gate_weight, first_block, local_blocks, 0)
    admit_weight = lax.dynamic_slice_in_dim(input_gate_weight, first_block, local_blocks, 0)
    u_blocks = recurrence_input.reshape(rows_dev, local_blocks, block_width)
    forget_gate = jax.nn.sigmoid(
        jnp.einsum(
            "tnb,nbc->tnc", u_blocks, recall_weight, preferred_element_type=jnp.float32
        ).reshape(rows_dev, channels)
    )
    admit_gate = jax.nn.sigmoid(
        jnp.einsum(
            "tnb,nbc->tnc", u_blocks, admit_weight, preferred_element_type=jnp.float32
        ).reshape(rows_dev, channels)
    )
    baseline_rate = jax.nn.softplus(-channel_decay_param)
    decay_logarithm = -8.0 * forget_gate * baseline_rate[None, :] + extra_log_decay
    decay_step = jnp.exp(decay_logarithm)
    input_scale = jnp.sqrt(-jnp.expm1(2.0 * decay_logarithm))
    u_float = recurrence_input.astype(jnp.float32)
    driven = u_float * admit_gate * input_scale
    recv_rows, recv_cot, states, prev_states = dispatch(
        send_rows.reshape(experts, capacity, feat_width),
        send_cot.reshape(experts, capacity, feat_width),
        decay_step,
        driven,
    )
    row_width = recv_rows.shape[2]
    grads = expert_step(
        recv_rows.reshape(-1, row_width),
        recv_cot.reshape(-1, row_width),
        (expert_gate_weight[0], expert_up_weight[0], expert_down_weight[0], recurrent_output_weight),
        pick_any.reshape(experts, capacity, rows_dev).transpose(0, 2, 1),
        output_gradient,
        (
            states,
            prev_states,
            decay_step,
            forget_gate,
            admit_gate,
            input_scale,
            recurrence_input,
            output_gate_logits,
            baseline_rate[None, :],
            recurrence_gate_weight,
            input_gate_weight,
        ),
    )
    grad_gate, grad_up, grad_down, grad_out_proj, grad_input, grad_gate_pre = grads
    return (
        grad_gate[None],
        grad_up[None],
        grad_down[None],
        grad_out_proj,
        grad_input,
        grad_gate_pre,
    )


def solution(mesh):
    placed = (
        P("sp", "tp"),
        P("sp", "tp"),
        P("sp", None),
        P("sp", None),
        P("sp", None, "tp"),
        P("sp", None, "tp"),
        P("sp", "tp", None),
        P(None, "tp"),
        P("sp", "tp"),
        P("sp", "tp"),
        P(),
        P(),
        P("tp"),
        P("sp", "tp"),
    )
    return jax.shard_map(
        per_device,
        mesh=mesh,
        in_specs=placed,
        out_specs=(
            P("sp", None, "tp"),
            P("sp", None, "tp"),
            P("sp", "tp", None),
            P("sp", "tp"),
            P("sp", "tp"),
            P("sp", "tp"),
        ),
        check_vma=False,
    )
```
